32 devices in a mesh: sp: 4 (over y, x), tp: 8 (over z, core).
Axes of the slice: x: 2, y: 2, z: 4, core: 2. Of those that a mesh axis runs over, the one named last changes fastest.
Arguments:
- stream: bfloat16 [8, 1536, 2048], P('tp', 'sp'), may hold values from -80 to 80
- norm_gain: float32 [2048], replicated, may hold values from 0.1 to 1.9
- w_lin: bfloat16 [1024, 2048], P('tp'), may hold values from -0.125 to 0.125
- w_gate: bfloat16 [1024, 2048], P('tp'), may hold values from -0.125 to 0.125
- conv_taps: bfloat16 [31, 1024], replicated, may hold values from -3 to 3
- conv_bias: float32 [1024], replicated, may hold values from -3 to 3
- ln_gain: float32 [1024], replicated, may hold values from 0.1 to 1.9
- ln_shift: float32 [1024], replicated, may hold values from -3 to 3
- w_proj: bfloat16 [1024, 2048], P('tp'), may hold values from -0.1875 to 0.1875
Outputs:
- result_stream: bfloat16 [8, 1536, 2048], P('tp', 'sp')
The draws below stay inside these ranges and needn't reach their ends.
All inputs are finite; a program needn't handle non-finite values.
Results may differ from the reference program's by a relative error of at most 0.0024.
Values may be sent and summed in bfloat16 or wider, within the bound.
A program may use at most 64 MiB of HBM per device.

```python
import jax
import jax.numpy as jnp
from jax import lax

D = 2048
CC = 1024
KW = 31
SEQ_LEN = 1536
SEQS = 8


def draw_stream(key, part):
    k_base, k_cols, k_rows = jax.random.split(jax.random.fold_in(key, 11), 3)
    cols = jnp.arange(D, dtype=jnp.float32) / D
    col_scale = jnp.exp(jnp.log(4.0) * cols) * jnp.exp(jax.random.uniform(k_cols, (D,), jnp.float32, -0.35, 0.35))
    row_scale = jnp.exp(jax.random.uniform(k_rows, (SEQS, SEQ_LEN, 1), jnp.float32, 0.0, jnp.log(10.0))) / 3.0
    base = jnp.clip(jax.random.normal(k_base, (SEQS, SEQ_LEN, D), jnp.float32), -4.0, 4.0)
    return (base * row_scale * col_scale).astype(jnp.bfloat16)


def draw_conv_taps(key, part):
    k_base, k_cols = jax.random.split(jax.random.fold_in(key, 23), 2)
    cols = jnp.arange(CC, dtype=jnp.float32) / CC
    col_scale = jnp.exp(jnp.log(3.0) * cols) * jnp.exp(jax.random.uniform(k_cols, (1, CC), jnp.float32, -0.35, 0.35))
    base = jnp.clip(jax.random.normal(k_base, (KW, CC), jnp.float32), -3.5, 3.5)
    return (base * col_scale * KW ** (-0.5)).astype(jnp.bfloat16)


def level_of(stream_key, dims, pieces, smallest, top_value):
    loudness = 1.0
    for dim, shards_of in pieces:
        draws = jax.random.uniform(jax.random.fold_in(jax.random.fold_in(stream_key, 6), dim), (shards_of,), jnp.float32, smallest / len(pieces), top_value / len(pieces))
        loudness = loudness * jnp.repeat(jnp.exp(draws), dims[dim] // shards_of).reshape((-1,) + (1,) * (len(dims) - 1 - dim))
    return loudness


def gaussian(key, shape, deviation, reach, cuts=(), kind=jnp.bfloat16):
    drawn = deviation * jax.random.normal(key, shape, jnp.float32)
    if cuts:
        drawn = drawn * level_of(key, shape, cuts, -0.22, 0.18)
    return jnp.clip(drawn, -reach, reach).astype(kind)


def setup_inputs(seed: int = 0) -> dict:
    seeds = jax.random.split(jax.random.key(seed), 10)
    return {
        "stream": draw_stream(jax.random.fold_in(seeds[9], 71), 0),
        "norm_gain": jnp.clip(1.0 + 0.18 * jax.random.normal(seeds[1], (D,), jnp.float32), 0.1, 1.9),
        "w_lin": gaussian(seeds[2], (CC, D), D ** -0.5, 0.125, ((0, 8),)),
        "w_gate": gaussian(seeds[3], (CC, D), D ** -0.5, 0.125, ((0, 8),)),
        "conv_taps": draw_conv_taps(jax.random.fold_in(seeds[9], 71), 0),
        "conv_bias": gaussian(seeds[5], (CC,), 0.5, 3.0, (), jnp.float32),
        "ln_gain": jnp.clip(1.0 + 0.18 * jax.random.normal(seeds[6], (CC,), jnp.float32), 0.1, 1.9),
        "ln_shift": gaussian(seeds[7], (CC,), 0.5, 3.0, (), jnp.float32),
        "w_proj": gaussian(seeds[8], (CC, D), CC ** -0.5, 0.1875, ((0, 8),)),
    }


EPS = 1e-06

def rms_rows(rows, gain):
    full = rows.astype(jnp.float32)
    scale = lax.rsqrt(lax.optimization_barrier(jnp.mean(full * full, axis=1, keepdims=True)) + EPS)
    return (full * scale * gain.astype(jnp.float32)).astype(jnp.bfloat16)

def project_rows(normed, weight):
    return lax.dot_general(normed, weight, (((1,), (1,)), ((), ())), preferred_element_type=jnp.float32)

def reference(stream, norm_gain, w_lin, w_gate, conv_taps, conv_bias, ln_gain, ln_shift, w_proj):
    taps_full = conv_taps.astype(jnp.float32)

    def one_sequence(current):
        normed = rms_rows(current, norm_gain)
        linear = project_rows(normed, w_lin)
        gating = project_rows(normed, w_gate)
        mixed = (linear * jax.nn.sigmoid(gating)).astype(jnp.bfloat16)
        length = current.shape[0]
        padded = jnp.pad(mixed.astype(jnp.float32), ((KW - 1, 0), (0, 0)))
        conv = jnp.zeros((length, mixed.shape[1]), jnp.float32)
        for tap in range(KW):
            conv = conv + taps_full[tap] * padded[tap:tap + length]
        conv = conv + conv_bias
        mean = lax.optimization_barrier(jnp.mean(conv, axis=1, keepdims=True))
        meansq = lax.optimization_barrier(jnp.mean(conv * conv, axis=1, keepdims=True))
        var = meansq - mean * mean
        activated = jax.nn.silu((conv - mean) * lax.rsqrt(var + EPS) * ln_gain + ln_shift).astype(jnp.bfloat16)
        projected = jnp.dot(activated, w_proj, preferred_element_type=jnp.float32)
        return (current.astype(jnp.float32) + projected).astype(jnp.bfloat16)
    return lax.map(one_sequence, stream)
```

```python
import functools

import jax
import jax.numpy as jnp
from jax import lax
from jax.experimental import pallas as pl
from jax.experimental.pallas import tpu as pltpu
from jax.sharding import PartitionSpec as P

EPS = 1e-06
HALO = 32
F32 = jnp.float32
BF16 = jnp.bfloat16
MESH = pl.DeviceIdType.MESH


def kernel(
    nsp, nz, kw,
    x_any, gain_any, wl_ref, wg_ref, wp_ref, taps_any, bias_any, lng_any, lnb_any,
    out_ref,
    x_ref, gain_ref, taps_ref, bias_ref, lng_ref, lnb_ref, held, xh, normed, mix, conv, act, taps,
    local_sem, halo_sem, z_recv, x_recv, y_recv, d_recv, up_send, dn_send, x_send, y_send, d_send, dp_recv, dp_send,
):
    rows, width = x_ref.shape
    block = held.shape[2]
    shard = block // 2
    lanes = min(128, block)
    strips = block // lanes
    quarter = width // 4
    half = quarter // 2
    p, tp = lax.axis_index("sp"), lax.axis_index("tp")
    z, c = tp // 2, tp % 2
    q = p % 4
    low, high = q % 2, q // 2
    beside = (p + 1 - 2 * low, tp)
    across = (p + 2 - 4 * high, tp)
    twin = (p, z * 2 + 1 - c)
    above = (p, tp + 2)
    below = (p, tp - 2)
    parity = (low + high) % 2
    has_up, has_dn = z < nz - 1, z > 0
    has_next, has_prev = p < nsp - 1, p > 0
    qx, qy, qd = q + 1 - 2 * low, q + 2 - 4 * high, 3 - q

    def cols(start, size):
        return pl.ds(pl.multiple_of(start, 128), size)

    def at(kind, src, core, start, size):
        return held.at[kind, src, pl.ds(pl.multiple_of(core * shard, 16), shard), cols(start, size)]

    def send(piece, ssem, rsem, target):
        return pltpu.make_async_remote_copy(
            src_ref=piece, dst_ref=piece, send_sem=ssem, recv_sem=rsem, device_id=target, device_id_type=MESH
        )

    def final(kind):
        return isinstance(kind, int) and kind == 2

    def z_piece(kind, src, i):
        if not final(kind):
            return at(kind, src, c, q * quarter, quarter)
        return at(kind, src, c, (parity * 2 + i) * quarter, quarter)

    def z_copy(kind, src, i, up):
        return send(
            z_piece(kind, src, i), (up_send if up else dn_send).at[kind, src, i], z_recv.at[kind, src, i],
            above if up else below,
        )

    def z_pieces(kind):
        return 2 if final(kind) else 1

    def x_copy(kind, src, i, incoming):
        if final(kind):
            piece = at(2, src, c, ((1 - parity if incoming else parity) * 2) * quarter, quarter)
        elif i == 0:
            piece = at(kind, src, c, (qx if incoming else q) * quarter, quarter)
        else:
            piece = at(kind, src, c, (qd if incoming else qy) * quarter, half)
        return send(piece, x_send.at[kind, src, i], x_recv.at[kind, src, i], beside)

    def y_copy(kind, src, i, incoming):
        if final(kind):
            piece = at(2, src, c, ((1 - parity if incoming else parity) * 2 + 1) * quarter, quarter)
        elif i == 0:
            piece = at(kind, src, c, (qy if incoming else q) * quarter, quarter)
        else:
            piece = at(kind, src, c, (qd if incoming else qx) * quarter + half, half)
        return send(piece, y_send.at[kind, src, i], y_recv.at[kind, src, i], across)

    def d_copy(kind, src, core):
        return send(at(kind, src, core, 0, width), d_send.at[kind, src], d_recv.at[kind, src], twin)

    def d_piece(kind, src, start, size):
        return send(at(kind, src, c, start, size), d_send.at[kind, src], d_recv.at[kind, src], twin)

    def p_cols(slot):
        return ((parity + slot // 2) % 2 * 2 + slot % 2) * quarter

    def p_copy(src, slot, core):
        return send(at(2, src, core, p_cols(slot), quarter), dp_send.at[src, slot], dp_recv.at[src, slot], twin)

    def halo_copy():
        return pltpu.make_async_remote_copy(
            src_ref=x_ref.at[pl.ds(rows - HALO, HALO)], dst_ref=xh, send_sem=halo_sem.at[0],
            recv_sem=halo_sem.at[1], device_id=(p + 1, tp), device_id_type=MESH,
        )

    mine = [
        pltpu.make_async_copy(ref, at(kind, z, c, 0, width), local_sem.at[kind])
        for kind, ref in enumerate((wl_ref, wg_ref, wp_ref))
    ]
    stream_in = pltpu.make_async_copy(x_any, x_ref, local_sem.at[3])
    mine[0].start()
    stream_in.start()
    mine[1].start()
    small = [
        pltpu.make_async_copy(ref, there, local_sem.at[4 + i])
        for i, (ref, there) in enumerate((
            (gain_any, gain_ref), (taps_any, taps_ref), (bias_any, bias_ref), (lng_any, lng_ref), (lnb_any, lnb_ref),
        ))
    ]
    for copy in small:
        copy.start()
    mine[2].start()

    barrier = pltpu.get_barrier_semaphore()
    for target in (beside, across, twin):
        pl.semaphore_signal(barrier, inc=1, device_id=target, device_id_type=MESH)
    for there, target in (
        (has_up, above), (has_dn, below), (has_next, (p + 1, tp)), (has_prev, (p - 1, tp)),
    ):
        @pl.when(there)
        def _():
            pl.semaphore_signal(barrier, inc=1, device_id=target, device_id_type=MESH)

    one = lambda there: jnp.where(there, 1, 0)
    pl.semaphore_wait(barrier, 3 + one(has_up) + one(has_dn) + one(has_next) + one(has_prev))

    def start_own(kind):
        for i in range(z_pieces(kind)):
            @pl.when(has_up)
            def _():
                z_copy(kind, z, i, True).start()

            @pl.when(has_dn)
            def _():
                z_copy(kind, z, i, False).start()

    mine[0].wait()
    start_own(0)
    mine[1].wait()
    start_own(1)
    stream_in.wait()

    @pl.when(has_next)
    def _():
        halo_copy().start()

    d_copy(0, z, c).start()
    d_copy(1, z, c).start()
    mine[2].wait()
    for slot in range(4):
        p_copy(z, slot, c).start()

    @pl.when(has_up & (z == 0))
    def _():
        for i in range(2):
            z_copy(2, z, i, True).start()

    @pl.when(has_dn & (z == nz - 1))
    def _():
        for i in range(2):
            z_copy(2, z, i, False).start()

    def each(t, body):
        for sign in (-1, 1):
            src = z + sign * t

            @pl.when((src >= 0) & (src < nz))
            def _():
                body(src, sign)

    def pass_on(kind, src, sign, i):
        z_copy(kind, src, i, True).wait_recv()
        if sign < 0:
            @pl.when(has_up)
            def _():
                z_copy(kind, src, i, True).start()
        else:
            @pl.when(has_dn)
            def _():
                z_copy(kind, src, i, False).start()

    def relay(kind):
        def body(src, sign):
            pass_on(kind, src, sign, 0)
            x_copy(kind, src, 0, False).start()
            y_copy(kind, src, 0, False).start()
            d_piece(kind, src, q * quarter, quarter).start()

        return body

    def onward(i):
        def body(src, sign):
            pass_on(2, src, sign, i)
            p_copy(src, i, c).start()

        return body

    def sideways(i):
        def body(src, sign):
            @pl.when(i == 0)
            def _():
                x_copy(2, src, 0, False).start()

            @pl.when(i == 1)
            def _():
                y_copy(2, src, 0, False).start()

        return body

    def diagonal(kind):
        def body(src, sign):
            x_copy(kind, src, 0, True).wait_recv()
            y_copy(kind, src, 1, False).start()
            d_piece(kind, src, qx * quarter, quarter).start()
            y_copy(kind, src, 0, True).wait_recv()
            x_copy(kind, src, 1, False).start()
            d_piece(kind, src, qy * quarter, quarter).start()

        return body

    def finish(kind):
        def body(src, sign):
            x_copy(kind, src, 1, True).wait_recv()
            d_piece(kind, src, qd * quarter, half).start()
            y_copy(kind, src, 1, True).wait_recv()
            d_piece(kind, src, qd * quarter + half, half).start()

        return body

    def arrived(src, sign):
        x_copy(2, src, 0, True).wait_recv()
        p_copy(src, 2, c).start()
        y_copy(2, src, 0, True).wait_recv()
        p_copy(src, 3, c).start()

    def norm_into(ref, base, count):
        @pl.loop(0, count // 16)
        def _(r):
            full = ref[pl.ds(pl.multiple_of(r * 16, 16), 16), :].astype(F32)
            scale = lax.rsqrt(jnp.mean(full * full, axis=1, keepdims=True) + EPS)
            normed[pl.ds(pl.multiple_of(base + r * 16, 16), 16), :] = (full * scale * gain_ref[...]).astype(BF16)

    for copy in small:
        copy.wait()
    norm_into(x_ref, HALO, rows)
    for i in range(nz):
        taps[i, 0:kw] = taps_ref[:, i * block:(i + 1) * block].astype(F32)
        taps[i, kw:kw + 1] = bias_ref[:, i * block:(i + 1) * block]

    @pl.when(has_prev)
    def _():
        halo_copy().wait_recv()

    @pl.when(jnp.logical_not(has_prev))
    def _():
        xh[...] = jnp.zeros_like(xh)

    norm_into(xh, 0, HALO)

    tile = 64
    lead = HALO - (kw - 1)
    nt = (((1,), (1,)), ((), ()))

    def on_planes(t, body):
        def one_side(side, carry):
            src = z + (2 * side - 1) * t
            valid = (src >= 0) & (src < nz) & ((t > 0) | (side == 0))

            @pl.when(valid)
            def _():
                body(side, src)

            return carry

        lax.fori_loop(0, 2, one_side, 0)

    def gate(t):
        def body(side, src):
            d_copy(0, src, 1 - c).wait_recv()
            d_copy(1, src, 1 - c).wait_recv()
            linear = lax.dot_general(normed[...], held[0, src], nt, preferred_element_type=F32)
            gating = lax.dot_general(normed[...], held[1, src], nt, preferred_element_type=F32)
            mixed = (linear * jax.nn.sigmoid(gating)).astype(BF16).astype(F32)
            for s in range(strips):
                mix[side, s, 0:HALO + rows] = mixed[:, s * lanes:(s + 1) * lanes]

        on_planes(t, body)

    def convolve(t):
        def body(side, src):
            @pl.loop(0, rows // tile)
            def _(r):
                base = pl.multiple_of(r * tile, tile)
                for s in range(strips):
                    lane = slice(s * lanes, (s + 1) * lanes)
                    total = jnp.broadcast_to(taps[src, kw:kw + 1, lane], (tile, lanes))
                    for b in range(8):
                        slab = mix[side, s, pl.ds(base + b, tile + HALO), :]
                        for a in range(HALO // 8 + 1):
                            tap = 8 * a + b - lead
                            if 0 <= tap < kw:
                                total = total + taps[src, tap:tap + 1, lane] * slab[8 * a:8 * a + tile]
                    conv[src, pl.ds(base, tile), lane] = total

        on_planes(t, body)

    slots = 2 * (nz - 1)

    @pl.loop(0, slots)
    def _(m):
        each(1 + m // 2, relay(m % 2))

        @pl.when((m % 2 == 1) & (1 + m // 2 == z) & has_up)
        def _():
            for i in range(2):
                z_copy(2, z, i, True).start()

        @pl.when((m % 2 == 1) & (1 + m // 2 == nz - 1 - z) & has_dn)
        def _():
            for i in range(2):
                z_copy(2, z, i, False).start()

        @pl.when(m >= 2)
        def _():
            each(m // 2, diagonal(m % 2))

        @pl.when(m == 0)
        def _():
            gate(0)

        @pl.when(m == 1)
        def _():
            convolve(0)

    @pl.loop(0, slots)
    def _(m):
        t, i = 1 + m // 2, m % 2
        each(t, onward(i))

        @pl.when(m < 2)
        def _():
            each(nz - 1, diagonal(i))

        @pl.when(m == 1)
        def _():
            each(1, sideways(0))
            each(1, sideways(1))

        @pl.when(m >= 2)
        def _():
            each(t, sideways(i))

        @pl.when(i == 0)
        def _():
            @pl.when(m > 0)
            def _():
                convolve(t - 1)

            each(t, finish(0))
            each(t, finish(1))

        @pl.when(i == 1)
        def _():
            gate(t)

    convolve(nz - 1)

    channels = nz * block

    @pl.loop(0, rows // 16)
    def _(r):
        here = pl.ds(pl.multiple_of(r * 16, 16), 16)
        parts = [conv[i, here, :] for i in range(nz)]
        mean = sum(jnp.sum(v, axis=1, keepdims=True) for v in parts) / channels
        meansq = sum(jnp.sum(v * v, axis=1, keepdims=True) for v in parts) / channels
        scale = lax.rsqrt(meansq - mean * mean + EPS)
        for i, v in enumerate(parts):
            lane = slice(i * block, (i + 1) * block)
            u = (v - mean) * scale * lng_ref[:, lane] + lnb_ref[:, lane]
            act[i, here, :] = (u * jax.nn.sigmoid(u)).astype(BF16)

    @pl.loop(0, 4)
    def _(n):
        @pl.when(n == 2)
        def _():
            @pl.loop(1, nz)
            def _(t):
                each(t, arrived)

        @pl.loop(0, nz)
        def _(src):
            p_copy(src, n, 1 - c).wait_recv()

        here = cols(p_cols(n), quarter)
        total = x_ref[:, here].astype(F32)
        for i in range(nz):
            total = total + jnp.dot(act[i], held[2, i, :, here], preferred_element_type=F32)
        out_ref[:, here] = total.astype(BF16)

    @pl.when(has_next)
    def _():
        halo_copy().wait_send()

    for kind in range(3):
        @pl.loop(0, nz)
        def _(src):
            if final(kind):
                for slot in range(4):
                    p_copy(src, slot, c).wait_send()
            else:
                d_copy(kind, src, c).wait_send()

            @pl.when(src != z)
            def _():
                for i in range(2 if kind < 2 else 1):
                    x_copy(kind, src, i, False).wait_send()
                    y_copy(kind, src, i, False).wait_send()

            for i in range(z_pieces(kind)):
                @pl.when((src <= z) & has_up)
                def _():
                    z_copy(kind, src, i, True).wait_send()

                @pl.when((src >= z) & has_dn)
                def _():
                    z_copy(kind, src, i, False).wait_send()


def local(nsp, ntp, stream, norm_gain, w_lin, w_gate, conv_taps, conv_bias, ln_gain, ln_shift, w_proj):
    _, rows, width = stream.shape
    kw, channels = conv_taps.shape
    nz = ntp // 2
    block = channels // nz
    lanes = min(128, block)
    kept = pl.BlockSpec(memory_space=pltpu.HBM)
    dma = pltpu.SemaphoreType.DMA
    out = pl.pallas_call(
        functools.partial(kernel, nsp, nz, kw),
        out_shape=pltpu.VMEM((rows, width), BF16),
        in_specs=[kept] * 9,
        out_specs=pl.BlockSpec(memory_space=pltpu.VMEM),
        scratch_shapes=[
            pltpu.VMEM((rows, width), BF16),
            pltpu.VMEM((1, width), F32),
            pltpu.VMEM((kw, channels), BF16),
            pltpu.VMEM((1, channels), F32),
            pltpu.VMEM((1, channels), F32),
            pltpu.VMEM((1, channels), F32),
            pltpu.VMEM((3, nz, block, width), BF16),
            pltpu.VMEM((HALO, width), BF16),
            pltpu.VMEM((HALO + rows, width), BF16),
            pltpu.VMEM((2, block // lanes, HALO + rows + 8, lanes), F32),
            pltpu.VMEM((nz, rows, block), F32),
            pltpu.VMEM((nz, rows, block), BF16),
            pltpu.VMEM((nz, kw + 1, block), F32),
            dma((9,)), dma((2,)),
            dma((3, nz, 2)), dma((3, nz, 2)), dma((3, nz, 2)), dma((3, nz)),
            dma((3, nz, 2)), dma((3, nz, 2)), dma((3, nz, 2)), dma((3, nz, 2)), dma((3, nz)), dma((nz, 4)), dma((nz, 4)),
        ],
        compiler_params=pltpu.CompilerParams(
            collective_id=0, has_side_effects=True, vmem_limit_bytes=60 * 1024 * 1024
        ),
    )(
        stream[0], norm_gain[None], w_lin, w_gate, w_proj, conv_taps,
        conv_bias[None], ln_gain[None], ln_shift[None],
    )
    return out[None]


def solution(mesh):
    placed = (
        P("tp", "sp", None), P(), P("tp", None), P("tp", None), P(), P(), P(), P(), P("tp", None),
    )
    return jax.shard_map(
        functools.partial(local, mesh.shape["sp"], mesh.shape["tp"]),
        mesh=mesh, in_specs=placed, out_specs=P("tp", "sp", None), check_vma=False,
    )
```

```python
import functools

import jax
import jax.numpy as jnp
from jax import lax
from jax.experimental import pallas as pl
from jax.experimental.pallas import tpu as pltpu
from jax.sharding import PartitionSpec as P

EPS = 1e-06
HALO = 32
F32 = jnp.float32
BF16 = jnp.bfloat16
MESH = pl.DeviceIdType.MESH


def kernel(
    nsp, nz, kw,
    x_any, gain_any, wl_ref, wg_ref, wp_ref, taps_any, bias_any, lng_any, lnb_any,
    out_ref,
    x_ref, gain_ref, taps_ref, bias_ref, lng_ref, lnb_ref, held, xh, normed, mix, conv, act, taps, acc,
    local_sem, halo_sem, z_recv, x_recv, y_recv, d_recv, up_send, dn_send, x_send, y_send, d_send, dp_recv,
):
    rows, width = x_ref.shape
    block = held.shape[2]
    shard = block // 2
    lanes = min(128, block)
    strips = block // lanes
    quarter = width // 4
    half = quarter // 2
    p, tp = lax.axis_index("sp"), lax.axis_index("tp")
    z, c = tp // 2, tp % 2
    q = p % 4
    low, high = q % 2, q // 2
    beside = (p + 1 - 2 * low, tp)
    across = (p + 2 - 4 * high, tp)
    twin = (p, z * 2 + 1 - c)
    above = (p, tp + 2)
    below = (p, tp - 2)
    has_up, has_dn = z < nz - 1, z > 0
    has_next, has_prev = p < nsp - 1, p > 0
    qx, qy, qd = q + 1 - 2 * low, q + 2 - 4 * high, 3 - q

    def cols(start, size):
        return pl.ds(pl.multiple_of(start, 128), size)

    def at(kind, src, core, start, size):
        return held.at[kind, src, pl.ds(pl.multiple_of(core * shard, 16), shard), cols(start, size)]

    def send(piece, ssem, rsem, target):
        return pltpu.make_async_remote_copy(
            src_ref=piece, dst_ref=piece, send_sem=ssem, recv_sem=rsem, device_id=target, device_id_type=MESH
        )

    def direct(kind, src):
        return (kind == 2) | ((kind == 1) & ((src == 0) | (src == nz - 1)))

    def full(kind, src):
        return (kind == 0) & (((src == 0) & (z == 1)) | ((src == nz - 1) & (z == nz - 2)))

    def z_copy(kind, src, i, up):
        return send(
            at(kind, src, c, (q, qd, qx, qy)[i] * quarter, quarter),
            (up_send if up else dn_send).at[kind, src, i], z_recv.at[kind, src, i], above if up else below,
        )

    def x_copy(kind, src, i, incoming):
        if i == 0:
            piece = at(kind, src, c, (qx if incoming else q) * quarter, quarter)
        else:
            piece = at(kind, src, c, (qd if incoming else qy) * quarter, half)
        return send(piece, x_send.at[kind, src, i], x_recv.at[kind, src, i], beside)

    def y_copy(kind, src, i, incoming):
        if i == 0:
            piece = at(kind, src, c, (qy if incoming else q) * quarter, quarter)
        else:
            piece = at(kind, src, c, (qd if incoming else qx) * quarter + half, half)
        return send(piece, y_send.at[kind, src, i], y_recv.at[kind, src, i], across)

    def d_copy(kind, src, core):
        return send(at(kind, src, core, 0, width), d_send, d_recv.at[kind, src], twin)

    def d_piece(kind, src, start, size):
        return send(at(kind, src, c, start, size), d_send, d_recv.at[kind, src], twin)

    def p_cols(slot):
        return (q, qx, qy, qd)[slot] * quarter

    def p_copy(src, slot, core):
        return send(at(2, src, core, p_cols(slot), quarter), d_send, dp_recv.at[src, slot], twin)

    def halo_copy():
        return pltpu.make_async_remote_copy(
            src_ref=x_ref.at[pl.ds(rows - HALO, HALO)], dst_ref=xh, send_sem=halo_sem.at[0],
            recv_sem=halo_sem.at[1], device_id=(p + 1, tp), device_id_type=MESH,
        )

    mine = [
        pltpu.make_async_copy(ref, at(kind, z, c, 0, width), local_sem.at[kind])
        for kind, ref in enumerate((wl_ref, wg_ref, wp_ref))
    ]
    stream_in = pltpu.make_async_copy(x_any, x_ref, local_sem.at[3])
    mine[0].start()
    stream_in.start()
    mine[1].start()
    small = [
        pltpu.make_async_copy(ref, there, local_sem.at[4 + i])
        for i, (ref, there) in enumerate((
            (gain_any, gain_ref), (taps_any, taps_ref), (bias_any, bias_ref), (lng_any, lng_ref), (lnb_any, lnb_ref),
        ))
    ]
    for copy in small:
        copy.start()
    mine[2].start()

    barrier = pltpu.get_barrier_semaphore()
    for target in (beside, across, twin):
        pl.semaphore_signal(barrier, inc=1, device_id=target, device_id_type=MESH)
    for there, target in (
        (has_up, above), (has_dn, below), (has_next, (p + 1, tp)), (has_prev, (p - 1, tp)),
    ):
        @pl.when(there)
        def _():
            pl.semaphore_signal(barrier, inc=1, device_id=target, device_id_type=MESH)

    one = lambda there: jnp.where(there, 1, 0)
    pl.semaphore_wait(barrier, 3 + one(has_up) + one(has_dn) + one(has_next) + one(has_prev))

    def start_own(kind, i, up):
        @pl.when(has_up if up else has_dn)
        def _():
            z_copy(kind, z, i, up).start()

    def start_ends(*pieces):
        for up, there in ((True, has_up & (z == 0)), (False, has_dn & (z == nz - 1))):
            @pl.when(there)
            def _():
                for kind, i in pieces:
                    z_copy(kind, z, i, up).start()

    mine[0].wait()
    start_own(0, 0, True)
    start_own(0, 0, False)
    mine[1].wait()
    start_own(1, 0, True)
    start_own(1, 0, False)
    start_ends((1, 1), (0, 1), (0, 2), (0, 3))
    stream_in.wait()

    @pl.when(has_next)
    def _():
        halo_copy().start()

    d_copy(0, z, c).start()
    d_copy(1, z, c).start()
    mine[2].wait()
    for slot in range(4):
        p_copy(z, slot, c).start()

    start_ends((2, 0), (2, 1))

    def each(t, body):
        for sign in (-1, 1):
            src = z + sign * t

            @pl.when((src >= 0) & (src < nz))
            def _():
                body(src, sign)

    def pass_on(kind, src, sign, i):
        z_copy(kind, src, i, True).wait_recv()
        if sign < 0:
            @pl.when(has_up)
            def _():
                z_copy(kind, src, i, True).start()
        else:
            @pl.when(has_dn)
            def _():
                z_copy(kind, src, i, False).start()

    def twin_piece(kind, src, slot):
        if isinstance(kind, int) and kind == 2:
            p_copy(src, slot, c).start()
        else:
            d_piece(kind, src, p_cols(slot), quarter).start()

    def sideways(kind):
        def body(src, sign):
            @pl.when(jnp.logical_not(full(kind, src)))
            def _():
                x_copy(kind, src, 0, False).start()
                y_copy(kind, src, 0, False).start()

        return body

    def relay(kind):
        def body(src, sign):
            pass_on(kind, src, sign, 0)
            twin_piece(kind, src, 0)

        return body

    def relay_far(kind):
        def body(src, sign):
            @pl.when(direct(kind, src))
            def _():
                pass_on(kind, src, sign, 1)
                twin_piece(kind, src, 3)

        return body

    def diagonal(kind):
        def body(src, sign):
            more = jnp.logical_not(direct(kind, src))

            @pl.when(jnp.logical_not(full(kind, src)))
            def _():
                x_copy(kind, src, 0, True).wait_recv()

                @pl.when(more)
                def _():
                    y_copy(kind, src, 1, False).start()

                twin_piece(kind, src, 1)
                y_copy(kind, src, 0, True).wait_recv()

                @pl.when(more)
                def _():
                    x_copy(kind, src, 1, False).start()

                twin_piece(kind, src, 2)

        return body

    def finish(kind):
        def body(src, sign):
            whole = full(kind, src)

            @pl.when(jnp.logical_not(direct(kind, src) | whole))
            def _():
                x_copy(kind, src, 1, True).wait_recv()
                d_piece(kind, src, qd * quarter, half).start()
                y_copy(kind, src, 1, True).wait_recv()
                d_piece(kind, src, qd * quarter + half, half).start()

            @pl.when(whole)
            def _():
                for i, slot in ((1, 3), (2, 1), (3, 2)):
                    z_copy(kind, src, i, True).wait_recv()
                    twin_piece(kind, src, slot)

        return body

    def norm_into(ref, base, count):
        @pl.loop(0, count // 16)
        def _(r):
            full = ref[pl.ds(pl.multiple_of(r * 16, 16), 16), :].astype(F32)
            scale = lax.rsqrt(jnp.mean(full * full, axis=1, keepdims=True) + EPS)
            normed[pl.ds(pl.multiple_of(base + r * 16, 16), 16), :] = (full * scale * gain_ref[...]).astype(BF16)

    for copy in small:
        copy.wait()
    norm_into(x_ref, HALO, rows)
    for i in range(nz):
        taps[i, 0:kw] = taps_ref[:, i * block:(i + 1) * block].astype(F32)
        taps[i, kw:kw + 1] = bias_ref[:, i * block:(i + 1) * block]

    @pl.when(has_prev)
    def _():
        halo_copy().wait_recv()

    @pl.when(jnp.logical_not(has_prev))
    def _():
        xh[...] = jnp.zeros_like(xh)

    norm_into(xh, 0, HALO)

    tile = 64
    lead = HALO - (kw - 1)
    nt = (((1,), (1,)), ((), ()))

    def on_planes(t, body):
        def one_side(side, carry):
            src = z + (2 * side - 1) * t
            valid = (src >= 0) & (src < nz) & ((t > 0) | (side == 0))

            @pl.when(valid)
            def _():
                body(side, src)

            return carry

        lax.fori_loop(0, 2, one_side, 0)

    def gate(t):
        def body(side, src):
            d_copy(0, src, 1 - c).wait_recv()
            d_copy(1, src, 1 - c).wait_recv()
            linear = lax.dot_general(normed[...], held[0, src], nt, preferred_element_type=F32)
            gating = lax.dot_general(normed[...], held[1, src], nt, preferred_element_type=F32)
            mixed = (linear * jax.nn.sigmoid(gating)).astype(BF16).astype(F32)
            for s in range(strips):
                mix[side, s, 0:HALO + rows] = mixed[:, s * lanes:(s + 1) * lanes]

        on_planes(t, body)

    def convolve(t):
        def body(side, src):
            @pl.loop(0, rows // tile)
            def _(r):
                base = pl.multiple_of(r * tile, tile)
                for s in range(strips):
                    lane = slice(s * lanes, (s + 1) * lanes)
                    total = jnp.broadcast_to(taps[src, kw:kw + 1, lane], (tile, lanes))
                    for b in range(8):
                        slab = mix[side, s, pl.ds(base + b, tile + HALO), :]
                        for a in range(HALO // 8 + 1):
                            tap = 8 * a + b - lead
                            if 0 <= tap < kw:
                                total = total + taps[src, tap:tap + 1, lane] * slab[8 * a:8 * a + tile]
                    conv[src, pl.ds(base, tile), lane] = total

        on_planes(t, body)

    slots = 2 * (nz - 1)

    def own_last(t, i):
        @pl.when((t == z) & has_up)
        def _():
            z_copy(2, z, i, True).start()

        @pl.when((t == nz - 1 - z) & has_dn)
        def _():
            z_copy(2, z, i, False).start()

    def at_slot(m, step):
        each(1 + m // 2, step(m % 2))

    def crossed(t):
        each(t, relay(2))
        each(t, sideways(2))
        own_last(t, 1)

    def over(first, last, body):
        @pl.loop(first, last)
        def _(t):
            body(t)

    at_slot(0, relay)
    at_slot(0, sideways)
    gate(0)
    at_slot(1, relay)
    at_slot(1, sideways)
    convolve(0)
    each(1, relay_far(1))
    own_last(1, 0)
    edge = (z == 0) | (z == nz - 1)

    def pairs(t):
        m = 2 * (t - 1)
        at_slot(m - 2, diagonal)
        at_slot(m, relay)
        at_slot(m, sideways)

        @pl.when(t > 2)
        def _():
            at_slot(m - 4, finish)
            at_slot(m - 3, finish)

    def odds(t):
        m = 2 * t - 1
        at_slot(m, relay)
        at_slot(m - 2, diagonal)
        at_slot(m, sideways)
        each(t, relay_far(1))
        own_last(t, 0)

    def later(t):
        @pl.when(t > 2)
        def _():
            gate(t - 2)
            convolve(t - 2)

    @pl.when(edge)
    def _():
        @pl.loop(2, nz - 1)
        def _(t):
            pairs(t)
            odds(t)
            later(t)

        pairs(nz - 1)
        at_slot(slots - 1, relay)
        at_slot(slots - 3, diagonal)
        at_slot(slots - 1, sideways)
        gate(nz - 3)
        each(nz - 1, relay_far(1))
        at_slot(slots - 2, diagonal)
        at_slot(slots - 4, finish)
        convolve(nz - 3)
        at_slot(slots - 3, finish)
        crossed(1)
        gate(nz - 2)
        crossed(2)
        at_slot(slots - 1, diagonal)
        convolve(nz - 2)
        at_slot(slots - 2, finish)
        over(3, nz, crossed)
        gate(nz - 1)
        convolve(nz - 1)

    @pl.when(jnp.logical_not(edge))
    def _():
        @pl.loop(2, nz - 1)
        def _(t):
            pairs(t)
            odds(t)
            later(t)

        at_slot(slots - 4, diagonal)
        at_slot(slots - 6, finish)
        crossed(1)
        at_slot(slots - 5, finish)
        gate(nz - 3)
        crossed(2)
        convolve(nz - 3)
        over(3, nz, crossed)
        at_slot(slots - 3, diagonal)
        at_slot(slots - 4, finish)
        each(1, relay_far(2))
        gate(nz - 2)
        over(2, nz, lambda t: each(t, relay_far(2)))
        convolve(nz - 2)

    channels = nz * block

    @pl.loop(0, rows // 16)
    def _(r):
        here = pl.ds(pl.multiple_of(r * 16, 16), 16)
        parts = [conv[i, here, :] for i in range(nz)]
        mean = sum(jnp.sum(v, axis=1, keepdims=True) for v in parts) / channels
        meansq = sum(jnp.sum(v * v, axis=1, keepdims=True) for v in parts) / channels
        scale = lax.rsqrt(meansq - mean * mean + EPS)
        for i, v in enumerate(parts):
            lane = slice(i * block, (i + 1) * block)
            u = (v - mean) * scale * lng_ref[:, lane] + lnb_ref[:, lane]
            act[i, here, :] = (u * jax.nn.sigmoid(u)).astype(BF16)

    def project(t, first):
        def body(side, src):
            for n in range(4):
                p_copy(src, n, 1 - c).wait_recv()
                here = cols(p_cols(n), quarter)
                before = x_ref[:, here].astype(F32) if first else acc[n]
                acc[n] = before + jnp.dot(act[src], held[2, src, :, here], preferred_element_type=F32)

        on_planes(t, body)

    def gather(t):
        @pl.when(edge)
        def _():
            each(t, relay_far(2))

        each(t, diagonal(2))

    gather(1)
    project(0, True)

    @pl.loop(1, nz - 2)
    def _(t):
        gather(t + 1)
        project(t, False)

    @pl.when(has_next)
    def _():
        halo_copy().wait_send()

    for kind in range(3):
        @pl.loop(0, nz)
        def _(src):
            far, whole = direct(kind, src), full(kind, src)

            @pl.when((src != z) & jnp.logical_not(whole))
            def _():
                x_copy(kind, src, 0, False).wait_send()
                y_copy(kind, src, 0, False).wait_send()

            @pl.when((src != z) & jnp.logical_not(far | whole))
            def _():
                x_copy(kind, src, 1, False).wait_send()
                y_copy(kind, src, 1, False).wait_send()

            for i in range(4 if kind == 0 else 2):
                goes = (i == 0) | far if kind else (i == 0) | ((src == z) & edge)

                @pl.when((src <= z) & has_up & goes)
                def _():
                    z_copy(kind, src, i, True).wait_send()

                @pl.when((src >= z) & has_dn & goes)
                def _():
                    z_copy(kind, src, i, False).wait_send()

    @pl.when(edge)
    def _():
        each(nz - 1, relay_far(2))

    project(nz - 2, False)
    each(nz - 1, diagonal(2))

    for n in (0, 3, 1, 2):
        here = cols(p_cols(n), quarter)
        src = nz - 1 - z

        @pl.when(edge)
        def _():
            p_copy(src, n, 1 - c).wait_recv()
            last = jnp.dot(act[src], held[2, src, :, here], preferred_element_type=F32)
            out_ref[:, here] = (acc[n] + last).astype(BF16)

        @pl.when(jnp.logical_not(edge))
        def _():
            out_ref[:, here] = acc[n].astype(BF16)

    sent = held.at[:, :, pl.ds(pl.multiple_of(c * shard, 16), shard)]
    send(sent, d_send, d_recv.at[0, 0], twin).wait_send()


def local(nsp, ntp, stream, norm_gain, w_lin, w_gate, conv_taps, conv_bias, ln_gain, ln_shift, w_proj):
    _, rows, width = stream.shape
    kw, channels = conv_taps.shape
    nz = ntp // 2
    block = channels // nz
    lanes = min(128, block)
    kept = pl.BlockSpec(memory_space=pltpu.HBM)
    dma = pltpu.SemaphoreType.DMA
    out = pl.pallas_call(
        functools.partial(kernel, nsp, nz, kw),
        out_shape=pltpu.VMEM((rows, width), BF16),
        in_specs=[kept] * 9,
        out_specs=pl.BlockSpec(memory_space=pltpu.VMEM),
        scratch_shapes=[
            pltpu.VMEM((rows, width), BF16),
            pltpu.VMEM((1, width), F32),
            pltpu.VMEM((kw, channels), BF16),
            pltpu.VMEM((1, channels), F32),
            pltpu.VMEM((1, channels), F32),
            pltpu.VMEM((1, channels), F32),
            pltpu.VMEM((3, nz, block, width), BF16),
            pltpu.VMEM((HALO, width), BF16),
            pltpu.VMEM((HALO + rows, width), BF16),
            pltpu.VMEM((2, block // lanes, HALO + rows + 8, lanes), F32),
            pltpu.VMEM((nz, rows, block), F32),
            pltpu.VMEM((nz, rows, block), BF16),
            pltpu.VMEM((nz, kw + 1, block), F32),
            pltpu.VMEM((4, rows, width // 4), F32),
            dma((9,)), dma((2,)),
            dma((3, nz, 4)), dma((3, nz, 2)), dma((3, nz, 2)), dma((3, nz)),
            dma((3, nz, 4)), dma((3, nz, 4)), dma((3, nz, 2)), dma((3, nz, 2)), dma, dma((nz, 4)),
        ],
        compiler_params=pltpu.CompilerParams(
            collective_id=0, has_side_effects=True, vmem_limit_bytes=60 * 1024 * 1024
        ),
    )(
        stream[0], norm_gain[None], w_lin, w_gate, w_proj, conv_taps,
        conv_bias[None], ln_gain[None], ln_shift[None],
    )
    return out[None]


def solution(mesh):
    placed = (
        P("tp", "sp", None), P(), P("tp", None), P("tp", None), P(), P(), P(), P(), P("tp", None),
    )
    return jax.shard_map(
        functools.partial(local, mesh.shape["sp"], mesh.shape["tp"]),
        mesh=mesh, in_specs=placed, out_specs=P("tp", "sp", None), check_vma=False,
    )
```

```python
import functools

import jax
import jax.numpy as jnp
from jax import lax
from jax.experimental import pallas as pl
from jax.experimental.pallas import tpu as pltpu
from jax.sharding import PartitionSpec as P

EPS = 1e-06
HALO = 32
F32 = jnp.float32
BF16 = jnp.bfloat16
MESH = pl.DeviceIdType.MESH


def kernel(
    nsp, nz, kw,
    x_any, gain_any, wl_ref, wg_ref, wp_ref, taps_any, bias_any, lng_any, lnb_any,
    out_ref,
    x_ref, gain_ref, taps_ref, bias_ref, lng_ref, lnb_ref, held, xh, normed, mix, conv, act, taps, acc, stat, power,
    local_sem, halo_sem, z_recv, z_first, z_rest, side_recv, corner_recv, d_recv, dp_recv, sent, d_send,
):
    rows, width = x_ref.shape
    block = held.shape[2]
    shard = block // 2
    lanes = min(128, block)
    strips = block // lanes
    quarter = width // 4
    half = quarter // 2
    p, tp = lax.axis_index("sp"), lax.axis_index("tp")
    z, c = tp // 2, tp % 2
    q = p % 4
    low, high = q % 2, q // 2
    beside = (p + 1 - 2 * low, tp)
    across = (p + 2 - 4 * high, tp)
    twin = (p, z * 2 + 1 - c)
    above = (p, tp + 2)
    below = (p, tp - 2)
    has_up, has_dn = z < nz - 1, z > 0
    has_next, has_prev = p < nsp - 1, p > 0
    edge = (z == 0) | (z == nz - 1)
    qx, qy, qd = q + 1 - 2 * low, q + 2 - 4 * high, 3 - q

    def cols(start, size):
        return pl.ds(pl.multiple_of(start, 128), size)

    def at(kind, src, core, start, size):
        return held.at[kind, src, pl.ds(pl.multiple_of(core * shard, 16), shard), cols(start, size)]

    def send(piece, ssem, rsem, target):
        return pltpu.make_async_remote_copy(
            src_ref=piece, dst_ref=piece, send_sem=ssem, recv_sem=rsem, device_id=target, device_id_type=MESH
        )

    def is_out(kind):
        return isinstance(kind, int) and kind == 2

    def direct(kind, src):
        return (kind == 2) | ((kind == 1) & ((src == 0) | (src == nz - 1)))

    def full(kind, src):
        return (kind == 0) & (((src == 0) & (z == 1)) | ((src == nz - 1) & (z == nz - 2)))

    def z_copy(kind, src, i, up):
        if isinstance(kind, int) and kind == 0 and i:
            arrived = z_rest
        else:
            arrived = z_recv.at[src, kind + i + (1 if is_out(kind) else 0)]
        return send(
            at(kind, src, c, (q, qd, qx, qy)[i] * quarter, quarter), sent.at[kind, src], arrived,
            above if up else below,
        )

    def part(ref, h):
        return ref.at[pl.ds(h * (shard // 2), shard // 2)]

    def first_copy(src, h, up, target, arrived):
        return send(part(at(0, src, c, q * quarter, quarter), h), sent.at[0, src], arrived, target)

    def x_copy(kind, src, i):
        piece = at(kind, src, c, q * quarter, quarter) if i == 0 else at(kind, src, c, qy * quarter, half)
        return send(piece, sent.at[kind, src], (corner_recv if i else side_recv).at[kind, src], beside)

    def y_copy(kind, src, i):
        piece = at(kind, src, c, q * quarter, quarter) if i == 0 else at(kind, src, c, qx * quarter + half, half)
        return send(piece, sent.at[kind, src], (corner_recv if i else side_recv).at[kind, src], across)

    def landed(kind, src, core, size, arrived):
        send(at(kind, src, core, 0, size), d_send, arrived, twin).wait_recv()

    def d_piece(kind, src, start, size):
        return send(at(kind, src, c, start, size), d_send, d_recv.at[src], twin)

    def is_last(src):
        return edge & (src == nz - 1 - z)

    def p_cols(slot):
        return (q, qx, qy, qd)[slot] * quarter

    def p_copy(src, slot):
        place = jnp.where(is_last(src), nz + slot, src)
        return send(at(2, src, c, p_cols(slot), quarter), d_send, dp_recv.at[place], twin)

    def halo_copy():
        return pltpu.make_async_remote_copy(
            src_ref=x_ref.at[pl.ds(rows - HALO, HALO)], dst_ref=xh, send_sem=halo_sem.at[0],
            recv_sem=halo_sem.at[1], device_id=(p + 1, tp), device_id_type=MESH,
        )

    barrier = pltpu.get_barrier_semaphore()
    for target in (beside, across, twin):
        pl.semaphore_signal(barrier, inc=1, device_id=target, device_id_type=MESH)
    for there, target in (
        (has_up, above), (has_dn, below), (has_next, (p + 1, tp)), (has_prev, (p - 1, tp)),
    ):
        @pl.when(there)
        def _():
            pl.semaphore_signal(barrier, inc=1, device_id=target, device_id_type=MESH)

    mine = [
        pltpu.make_async_copy(ref, at(kind, z, c, 0, width), local_sem.at[kind])
        for kind, ref in enumerate((wl_ref, wg_ref, wp_ref))
    ]
    stream_in = pltpu.make_async_copy(x_any, x_ref, local_sem.at[3])
    mine[0].start()
    stream_in.start()
    mine[1].start()
    small = [
        pltpu.make_async_copy(ref, there, local_sem.at[4 + i])
        for i, (ref, there) in enumerate((
            (gain_any, gain_ref), (taps_any, taps_ref), (bias_any, bias_ref), (lng_any, lng_ref), (lnb_any, lnb_ref),
        ))
    ]
    for copy in small:
        copy.start()
    mine[2].start()

    one = lambda there: jnp.where(there, 1, 0)
    pl.semaphore_wait(barrier, 3 + one(has_up) + one(has_dn) + one(has_next) + one(has_prev))

    def start_own(kind, i, up):
        @pl.when(has_up if up else has_dn)
        def _():
            z_copy(kind, z, i, up).start()

    def start_ends(*pieces):
        for up, there in ((True, has_up & (z == 0)), (False, has_dn & (z == nz - 1))):
            @pl.when(there)
            def _():
                for kind, i in pieces:
                    z_copy(kind, z, i, up).start()

    mine[0].wait()
    for h in range(2):
        for up, there in ((True, has_up), (False, has_dn)):
            @pl.when(there)
            def _():
                first_copy(z, h, up, above if up else below, z_first.at[0 if up else 1, h]).start()

    mine[1].wait()
    start_own(1, 0, True)
    start_own(1, 0, False)
    start_ends((1, 1), (0, 1), (0, 2), (0, 3))
    stream_in.wait()

    @pl.when(has_next)
    def _():
        halo_copy().start()

    d_piece(0, z, 0, width).start()
    d_piece(1, z, 0, width).start()
    mine[2].wait()
    for slot in range(4):
        p_copy(z, slot).start()

    start_ends((2, 0), (2, 1))

    def each(t, body):
        for sign in (-1, 1):
            src = z + sign * t

            @pl.when((src >= 0) & (src < nz))
            def _():
                body(src, sign)

    def pass_on(kind, src, sign, i):
        z_copy(kind, src, i, True).wait_recv()
        if sign < 0:
            @pl.when(has_up)
            def _():
                z_copy(kind, src, i, True).start()
        else:
            @pl.when(has_dn)
            def _():
                z_copy(kind, src, i, False).start()

    def twin_piece(kind, src, slot):
        if is_out(kind):
            p_copy(src, slot).start()
        else:
            d_piece(kind, src, p_cols(slot), quarter).start()

    def sideways(kind):
        def body(src, sign):
            @pl.when(jnp.logical_not(full(kind, src)))
            def _():
                x_copy(kind, src, 0).start()
                y_copy(kind, src, 0).start()

        return body

    def relay(kind):
        def body(src, sign):
            pass_on(kind, src, sign, 0)
            twin_piece(kind, src, 0)

        return body

    def relay_far(kind):
        def body(src, sign):
            @pl.when(direct(kind, src))
            def _():
                pass_on(kind, src, sign, 1)
                twin_piece(kind, src, 3)

        return body

    def first_relay(src, sign):
        for h in range(2):
            first_copy(src, h, True, above, z_first.at[0 if sign < 0 else 1, h]).wait_recv()
            onward, target = (has_up, above) if sign < 0 else (has_dn, below)

            @pl.when(onward)
            def _():
                first_copy(src, h, True, target, z_recv.at[src, 0]).start()

            @pl.when(jnp.logical_not(full(0, src)))
            def _():
                for target in (beside, across):
                    first_copy(src, h, True, target, side_recv.at[0, src]).start()

            send(part(at(0, src, c, q * quarter, quarter), h), d_send, d_recv.at[src], twin).start()

    def diagonal(kind):
        def body(src, sign):
            @pl.when(jnp.logical_not(full(kind, src)))
            def _():
                landed(kind, src, c, 2 * quarter, side_recv.at[kind, src])

                if not is_out(kind):
                    @pl.when(jnp.logical_not(direct(kind, src)))
                    def _():
                        y_copy(kind, src, 1).start()
                        x_copy(kind, src, 1).start()

                twin_piece(kind, src, 1)
                twin_piece(kind, src, 2)

        return body

    def finish(kind):
        def body(src, sign):
            whole = full(kind, src)

            @pl.when(jnp.logical_not(direct(kind, src) | whole))
            def _():
                landed(kind, src, c, quarter, corner_recv.at[kind, src])
                twin_piece(kind, src, 3)

            @pl.when(whole)
            def _():
                landed(kind, src, c, 3 * quarter, z_rest)
                for slot in range(1, 4):
                    twin_piece(kind, src, slot)

        return body

    def norm_into(ref, base, count):
        spans = [slice(i * 128, (i + 1) * 128) for i in range(width // 128)]

        def there(r):
            return pl.ds(pl.multiple_of(base + r * 16, 16), 16)

        @pl.loop(0, count // 16)
        def _(r):
            total = jnp.zeros((16, 128), F32)
            for span in spans:
                full = ref[pl.ds(pl.multiple_of(r * 16, 16), 16), span].astype(F32)
                total = total + full * full
            power[there(r), :] = total

        whole = slice(base, base + count)
        mean = jnp.sum(power[whole, :], axis=1, keepdims=True) / width
        power[whole, :] = jnp.broadcast_to(lax.rsqrt(mean + EPS), (count, 128))

        @pl.loop(0, count // 16)
        def _(r):
            scale = power[there(r), :]
            for span in spans:
                full = ref[pl.ds(pl.multiple_of(r * 16, 16), 16), span].astype(F32)
                normed[there(r), span] = (full * scale * gain_ref[:, span]).astype(BF16)

    for copy in small:
        copy.wait()
    stat[...] = jnp.zeros_like(stat)
    norm_into(x_ref, HALO, rows)
    for i in range(nz):
        taps[i, 0:kw] = taps_ref[:, i * block:(i + 1) * block].astype(F32)
        taps[i, kw:kw + 1] = bias_ref[:, i * block:(i + 1) * block]

    @pl.when(has_prev)
    def _():
        halo_copy().wait_recv()

    @pl.when(jnp.logical_not(has_prev))
    def _():
        xh[...] = jnp.zeros_like(xh)

    norm_into(xh, 0, HALO)

    tile = 64
    lead = HALO - (kw - 1)
    nt = (((1,), (1,)), ((), ()))

    def on_planes(t, body):
        def one_side(side, carry):
            src = z + (2 * side - 1) * t
            valid = (src >= 0) & (src < nz) & ((t > 0) | (side == 0))

            @pl.when(valid)
            def _():
                body(side, src)

            return carry

        lax.fori_loop(0, 2, one_side, 0)

    def gate(t):
        def body(side, src):
            pair = held.at[0:2, src, pl.ds(pl.multiple_of((1 - c) * shard, 16), shard)]
            send(pair, d_send, d_recv.at[src], twin).wait_recv()
            linear = lax.dot_general(normed[...], held[0, src], nt, preferred_element_type=F32)
            gating = lax.dot_general(normed[...], held[1, src], nt, preferred_element_type=F32)
            mixed = (linear * jax.nn.sigmoid(gating)).astype(BF16).astype(F32)
            for s in range(strips):
                mix[side, s, 0:HALO + rows] = mixed[:, s * lanes:(s + 1) * lanes]

        on_planes(t, body)

    def convolve(t):
        def body(side, src):
            @pl.loop(0, rows // tile)
            def _(r):
                base = pl.multiple_of(r * tile, tile)
                line, square = stat[0, pl.ds(base, tile), :], stat[1, pl.ds(base, tile), :]
                for s in range(strips):
                    lane = slice(s * lanes, (s + 1) * lanes)
                    total = jnp.broadcast_to(taps[src, kw:kw + 1, lane], (tile, lanes))
                    for b in range(8):
                        slab = mix[side, s, pl.ds(base + b, tile + HALO), :]
                        for a in range(HALO // 8 + 1):
                            tap = 8 * a + b - lead
                            if 0 <= tap < kw:
                                total = total + taps[src, tap:tap + 1, lane] * slab[8 * a:8 * a + tile]
                    conv[src, pl.ds(base, tile), lane] = total
                    line = line + total
                    square = square + total * total
                stat[0, pl.ds(base, tile), :] = line
                stat[1, pl.ds(base, tile), :] = square

        on_planes(t, body)

    slots = 2 * (nz - 1)

    def own_last(t, i):
        @pl.when((t == z) & has_up)
        def _():
            z_copy(2, z, i, True).start()

        @pl.when((t == nz - 1 - z) & has_dn)
        def _():
            z_copy(2, z, i, False).start()

    def at_slot(m, step):
        each(1 + m // 2, step(m % 2))

    def crossed(t):
        each(t, relay(2))
        each(t, sideways(2))
        own_last(t, 1)

    def over(first, last, body):
        @pl.loop(first, last)
        def _(t):
            body(t)

    each(1, first_relay)
    gate(0)
    at_slot(1, relay)
    at_slot(1, sideways)
    convolve(0)
    each(1, relay_far(1))
    own_last(1, 0)

    def pairs(t):
        m = 2 * (t - 1)
        at_slot(m - 2, diagonal)
        at_slot(m, relay)
        at_slot(m, sideways)

        @pl.when(t > 2)
        def _():
            at_slot(m - 4, finish)
            at_slot(m - 3, finish)

    def odds(t):
        m = 2 * t - 1
        at_slot(m, relay)
        at_slot(m - 2, diagonal)
        at_slot(m, sideways)
        each(t, relay_far(1))
        own_last(t, 0)

    def later(t):
        @pl.when(t > 2)
        def _():
            gate(t - 2)
            convolve(t - 2)

    @pl.when(edge)
    def _():
        @pl.loop(2, nz - 1)
        def _(t):
            pairs(t)
            odds(t)
            later(t)

        pairs(nz - 1)
        at_slot(slots - 1, relay)
        at_slot(slots - 3, diagonal)
        at_slot(slots - 1, sideways)
        gate(nz - 3)
        each(nz - 1, relay_far(1))
        at_slot(slots - 2, diagonal)
        at_slot(slots - 4, finish)
        convolve(nz - 3)
        at_slot(slots - 3, finish)
        crossed(1)
        crossed(2)
        gate(nz - 2)
        at_slot(slots - 1, diagonal)
        convolve(nz - 2)
        at_slot(slots - 2, finish)
        over(3, nz, crossed)
        gate(nz - 1)
        convolve(nz - 1)

    @pl.when(jnp.logical_not(edge))
    def _():
        @pl.loop(2, nz - 1)
        def _(t):
            pairs(t)
            odds(t)
            later(t)

        at_slot(slots - 4, diagonal)
        at_slot(slots - 6, finish)
        crossed(1)
        at_slot(slots - 5, finish)
        gate(nz - 3)
        crossed(2)
        convolve(nz - 3)
        over(3, nz, crossed)
        at_slot(slots - 3, diagonal)
        at_slot(slots - 4, finish)
        each(1, relay_far(2))
        gate(nz - 2)
        over(2, nz, lambda t: each(t, relay_far(2)))
        convolve(nz - 2)

    channels = nz * block
    mean = jnp.sum(stat[0], axis=1, keepdims=True) / channels
    meansq = jnp.sum(stat[1], axis=1, keepdims=True) / channels
    stat[0] = jnp.broadcast_to(mean, stat.shape[1:])
    stat[1] = jnp.broadcast_to(lax.rsqrt(meansq - mean * mean + EPS), stat.shape[1:])

    @pl.loop(0, rows // 16)
    def _(r):
        here = pl.ds(pl.multiple_of(r * 16, 16), 16)
        for i in range(nz):
            for s in range(strips):
                lane = slice(s * lanes, (s + 1) * lanes)
                both = slice(i * block + s * lanes, i * block + (s + 1) * lanes)
                u = (conv[i, here, lane] - stat[0, here, :]) * stat[1, here, :] * lng_ref[:, both] + lnb_ref[:, both]
                act[i, here, lane] = (u * jax.nn.sigmoid(u)).astype(BF16)

    def ready(src):
        landed(2, src, 1 - c, width, dp_recv.at[src])

    def products(srcs, here):
        return sum(jnp.dot(act[src], held[2, src, :, here], preferred_element_type=F32) for src in srcs)

    def project(srcs, first):
        for src in srcs:
            ready(src)
        for n in range(4):
            here = cols(p_cols(n), quarter)
            before = x_ref[:, here].astype(F32) if first else acc[n]
            acc[n] = before + products(srcs, here)

    def gather(t):
        @pl.when(edge)
        def _():
            each(t, relay_far(2))

        each(t, diagonal(2))

    def drain(kind):
        @pl.loop(0, nz)
        def _(src):
            far, own, passed = direct(kind, src) * 1, (src == z), ((src < z) & has_up) | ((src > z) & has_dn)
            other = jnp.where(full(kind, src), 0, 3 - far) + passed * (1 + far)
            mine = edge * (4, 2, 2)[kind] + (1 - edge * 1) * 2 * (1, 1, 2)[kind]
            count = jnp.where(own, mine, other)
            for n in range(1, 5):
                @pl.when(count == n)
                def _():
                    send(at(kind, src, c, 0, n * quarter), sent.at[kind, src], d_send, twin).wait_send()

    def inward(t):
        return jnp.where(z == 0, t, nz - 1 - t)

    near_edge = (z == 1) | (z == nz - 2)
    beyond = jnp.where(z == 1, nz - 1, 0)

    def finalize(srcs, n):
        here = cols(p_cols(n), quarter)
        out_ref[:, here] = (acc[n] + products(srcs, here)).astype(BF16) if srcs else acc[n].astype(BF16)

    gather(1)
    if nz == 4:
        gather(2)

    @pl.when(edge)
    def _():
        project([z, inward(1)], True)

    @pl.when(jnp.logical_not(edge))
    def _():
        project([z, z - 1, z + 1], True)

    drain(0)
    drain(1)

    @pl.loop(2, nz - 2)
    def _(t):
        gather(t)
        each(t, lambda src, sign: project([src], False))

    if nz > 4:
        gather(nz - 2)

    @pl.when(edge)
    def _():
        lasts = [inward(nz - 2), inward(nz - 1)]

        def complete(n):
            landed(2, inward(nz - 1), 1 - c, quarter, dp_recv.at[nz + n])
            finalize(lasts, n)

        each(nz - 1, relay_far(2))
        ready(inward(nz - 2))
        complete(0)
        each(nz - 1, diagonal(2))
        complete(3)
        complete(1)
        complete(2)

    @pl.when(near_edge)
    def _():
        ready(beyond)
        for n in range(4):
            finalize([beyond], n)

    if nz > 4:
        @pl.when(jnp.logical_not(edge | near_edge))
        def _():
            for n in range(4):
                finalize([], n)

    drain(2)

    @pl.when(has_next)
    def _():
        halo_copy().wait_send()

    passed_on = held.at[:, :, pl.ds(pl.multiple_of(c * shard, 16), shard)]
    send(passed_on, d_send, d_recv.at[0], twin).wait_send()


def local(nsp, ntp, stream, norm_gain, w_lin, w_gate, conv_taps, conv_bias, ln_gain, ln_shift, w_proj):
    _, rows, width = stream.shape
    kw, channels = conv_taps.shape
    nz = ntp // 2
    block = channels // nz
    lanes = min(128, block)
    kept = pl.BlockSpec(memory_space=pltpu.HBM)
    dma = pltpu.SemaphoreType.DMA
    out = pl.pallas_call(
        functools.partial(kernel, nsp, nz, kw),
        out_shape=pltpu.VMEM((rows, width), BF16),
        in_specs=[kept] * 9,
        out_specs=pl.BlockSpec(memory_space=pltpu.VMEM),
        scratch_shapes=[
            pltpu.VMEM((rows, width), BF16),
            pltpu.VMEM((1, width), F32),
            pltpu.VMEM((kw, channels), BF16),
            pltpu.VMEM((1, channels), F32),
            pltpu.VMEM((1, channels), F32),
            pltpu.VMEM((1, channels), F32),
            pltpu.VMEM((3, nz, block, width), BF16),
            pltpu.VMEM((HALO, width), BF16),
            pltpu.VMEM((HALO + rows, width), BF16),
            pltpu.VMEM((2, block // lanes, HALO + rows + 8, lanes), F32),
            pltpu.VMEM((nz, rows, block), F32),
            pltpu.VMEM((nz, rows, block), BF16),
            pltpu.VMEM((nz, kw + 1, block), F32),
            pltpu.VMEM((4, rows, width // 4), F32),
            pltpu.VMEM((2, rows, lanes), F32),
            pltpu.VMEM((HALO + rows, 128), F32),
            dma((9,)), dma((2,)),
            dma((nz, 5)), dma((2, 2)), dma, dma((3, nz)), dma((2, nz)), dma((nz,)), dma((nz + 4,)), dma((3, nz)), dma,
        ],
        compiler_params=pltpu.CompilerParams(
            collective_id=0, has_side_effects=True, vmem_limit_bytes=60 * 1024 * 1024
        ),
    )(
        stream[0], norm_gain[None], w_lin, w_gate, w_proj, conv_taps,
        conv_bias[None], ln_gain[None], ln_shift[None],
    )
    return out[None]


def solution(mesh):
    placed = (
        P("tp", "sp", None), P(), P("tp", None), P("tp", None), P(), P(), P(), P(), P("tp", None),
    )
    return jax.shard_map(
        functools.partial(local, mesh.shape["sp"], mesh.shape["tp"]),
        mesh=mesh, in_specs=placed, out_specs=P("tp", "sp", None), check_vma=False,
    )
```
